32 devices in a mesh: sp: 16 (over z, y, x), tp: 2 (over core).
Axes of the slice: x: 2, y: 2, z: 4, core: 2. Of those that a mesh axis runs over, the one named last changes fastest.
Arguments:
- queries: bfloat16 [4096, 1024], P('sp', 'tp'), may hold values from -6 to 6
- keys: bfloat16 [4096, 512], P('sp', 'tp'), may hold values from -6 to 6
- values: bfloat16 [4096, 512], P('sp', 'tp'), may hold values from -6 to 6
- q_gain: float32 [64], replicated, may hold values from 1.6 to 4.5
- key_norm_gain: float32 [64], replicated, may hold values from 1.6 to 4.5
- out_weight: bfloat16 [1024, 2048], P('tp'), may hold values from -0.1875 to 0.1875
- residual: bfloat16 [4096, 2048], P('sp'), may hold values from -6 to 6
- ln1_gain: float32 [2048], replicated, may hold values from 0.1 to 1.9
- ln1_bias: float32 [2048], replicated, may hold values from -3 to 3
- up_weight: bfloat16 [2048, 8192], P('sp', 'tp'), may hold values from -0.125 to 0.125
- down_weight: bfloat16 [8192, 2048], P('tp', 'sp'), may hold values from -0.0625 to 0.0625
- ln2_gain: float32 [2048], replicated, may hold values from 0.1 to 1.9
- ln2_bias: float32 [2048], replicated, may hold values from -3 to 3
Outputs:
- encoded: bfloat16 [4096, 2048], P('sp', 'tp')
The draws below stay inside these ranges and needn't reach their ends.
All inputs are finite; a program needn't handle non-finite values.
Results may differ from the reference program's by a relative error of at most 0.014.
Values may be sent and summed in bfloat16 or wider, within the bound.
A program may use at most 128 MiB of HBM per device.

```python
import math
import jax
import jax.numpy as jnp
from jax import lax

D = 2048
FF = 8192
QUERY_HEADS = 16
KEY_VALUE_HEADS = 8
HEAD_SIZE = 64
GRID_W = 64
SEQUENCE_TOKENS = 4096
N_TP = 2


def random_base_keys(key):
    return jnp.clip(jax.random.normal(jax.random.fold_in(key, 11), (SEQUENCE_TOKENS, KEY_VALUE_HEADS * HEAD_SIZE), jnp.float32), -6.0, 6.0)


def draw_keys(key, part):
    return random_base_keys(key).astype(jnp.bfloat16)


def draw_queries(key, part):
    drawn_q = jnp.clip(jax.random.normal(jax.random.fold_in(key, 12), (SEQUENCE_TOKENS, QUERY_HEADS * HEAD_SIZE), jnp.float32), -6.0, 6.0)
    return drawn_q.astype(jnp.bfloat16)


def draw_q_gain(key, part):
    return jax.random.uniform(jax.random.fold_in(key, 21), (HEAD_SIZE,), jnp.float32, 1.6, 2.4)


def draw_key_norm_gain(key, part):
    return jax.random.uniform(jax.random.fold_in(key, 22), (HEAD_SIZE,), jnp.float32, 1.6, 2.4)


def block_levels(rng, extent, cuts, least, high):
    level, own = 1.0, jax.random.fold_in(rng, 6)
    for dim, blocks in cuts:
        heights = jnp.exp(jax.random.uniform(jax.random.fold_in(own, dim), (blocks,), jnp.float32, least / len(cuts), high / len(cuts)))
        level = level * jnp.repeat(heights, extent[dim] // blocks).reshape([-1 if axis == dim else 1 for axis in range(len(extent))])
    return level


def gaussian(key, extent, scale, limit, shards=(), kind=jnp.bfloat16):
    values = jax.random.normal(key, extent, jnp.float32) * scale
    if len(shards) > 0:
        values = block_levels(key, extent, shards, -0.22, 0.18) * values
    return jnp.clip(values, min=-limit, max=limit).astype(kind)


def setup_inputs(seed: int = 0) -> dict:
    key_list = jax.random.split(jax.random.key(seed), 14)
    return {
        "queries": draw_queries(jax.random.fold_in(key_list[13], 71), 0),
        "keys": draw_keys(jax.random.fold_in(key_list[13], 71), 0),
        "values": gaussian(key_list[2], (SEQUENCE_TOKENS, KEY_VALUE_HEADS * HEAD_SIZE), 1.0, 6.0, ((0, 16), (1, 2))),
        "q_gain": draw_q_gain(jax.random.fold_in(key_list[13], 71), 0),
        "key_norm_gain": draw_key_norm_gain(jax.random.fold_in(key_list[13], 71), 0),
        "out_weight": gaussian(key_list[5], (QUERY_HEADS * HEAD_SIZE, D), (QUERY_HEADS * HEAD_SIZE) ** -0.5, 0.1875, ((0, 2),)),
        "residual": gaussian(key_list[6], (SEQUENCE_TOKENS, D), 1.0, 6.0, ((0, 16),)),
        "ln1_gain": jnp.clip(1.0 + 0.18 * jax.random.normal(key_list[7], (D,), jnp.float32), 0.1, 1.9),
        "ln1_bias": gaussian(key_list[8], (D,), 0.3, 3.0, (), jnp.float32),
        "up_weight": gaussian(key_list[9], (D, FF), D ** -0.5, 0.125, ((0, 16), (1, 2))),
        "down_weight": gaussian(key_list[10], (FF, D), FF ** -0.5, 0.0625, ((0, 2), (1, 16))),
        "ln2_gain": jnp.clip(1.0 + 0.18 * jax.random.normal(key_list[11], (D,), jnp.float32), 0.1, 1.9),
        "ln2_bias": gaussian(key_list[12], (D,), 0.3, 3.0, (), jnp.float32),
    }


ALPHA = 8.0 ** 0.25
ROTARY_BASE = 10000.0
RMS_EPSILON = 1e-06
NORM_EPSILON = 1e-05

def rotate_grid(heads_in, grid_places):
    half_dim = heads_in.shape[-1] // 2
    quarter = half_dim // 2
    inverse = ROTARY_BASE ** (-jnp.arange(quarter, dtype=jnp.float32) / quarter)

    def spin(segment, coords):
        angles = coords.astype(jnp.float32)[:, None] * inverse[None, :]
        cos_val = jnp.cos(angles)[:, None, :]
        sin_val = jnp.sin(angles)[:, None, :]
        lead_half = segment[..., :quarter]
        tail_half = segment[..., quarter:]
        return jnp.concatenate([lead_half * cos_val - tail_half * sin_val, tail_half * cos_val + lead_half * sin_val], -1)
    return jnp.concatenate([spin(heads_in[..., :half_dim], grid_places // GRID_W), spin(heads_in[..., half_dim:], grid_places % GRID_W)], -1)

def prepare_inputs(heads_in, gain_vec, grid_places, factor):
    values32 = heads_in.astype(jnp.float32)
    normed = values32 * lax.rsqrt(lax.optimization_barrier(jnp.mean(values32 * values32, -1, keepdims=True)) + RMS_EPSILON) * gain_vec
    return (rotate_grid(normed, grid_places) * factor).astype(jnp.bfloat16)

def layer_norm(pre_norm, gain_vec, bias_vec):
    row_mean = lax.optimization_barrier(jnp.mean(pre_norm, -1, keepdims=True))
    centred = pre_norm - row_mean
    spread = lax.optimization_barrier(jnp.mean(centred * centred, -1, keepdims=True))
    return centred * lax.rsqrt(spread + NORM_EPSILON) * gain_vec + bias_vec

def sum_partials(left_side, right_side):
    group_width = left_side.shape[1] // N_TP
    totals = jnp.zeros((left_side.shape[0], right_side.shape[1]), jnp.float32)
    for member in range(N_TP):
        partial_value = jnp.dot(left_side[:, member * group_width:(member + 1) * group_width], right_side[member * group_width:(member + 1) * group_width], preferred_element_type=jnp.float32)
        totals = totals + lax.optimization_barrier(partial_value.astype(jnp.bfloat16)).astype(jnp.float32)
    return totals

def reference(queries, keys, values, q_gain, key_norm_gain, out_weight, residual, ln1_gain, ln1_bias, up_weight, down_weight, ln2_gain, ln2_bias):
    sequence_length = queries.shape[0]
    grid_places = jnp.arange(sequence_length, dtype=jnp.int32)
    group_count_size = QUERY_HEADS // KEY_VALUE_HEADS
    single_query_block = math.gcd(sequence_length, 128)
    query_head_rows = prepare_inputs(queries.reshape(sequence_length, QUERY_HEADS, HEAD_SIZE), q_gain, grid_places, HEAD_SIZE ** (-0.5))
    key_head_rows = prepare_inputs(keys.reshape(sequence_length, KEY_VALUE_HEADS, HEAD_SIZE), key_norm_gain, grid_places, 1.0).astype(jnp.float32)
    value_head_rows = values.reshape(sequence_length, KEY_VALUE_HEADS, HEAD_SIZE).astype(jnp.float32)
    query_block_list = query_head_rows.reshape(sequence_length // single_query_block, single_query_block, KEY_VALUE_HEADS, group_count_size, HEAD_SIZE)

    def attend(q_block):
        scores = jnp.einsum('qhgd,khd->hgqk', q_block.astype(jnp.float32), key_head_rows)
        maxima = lax.optimization_barrier(jnp.max(scores, -1, keepdims=True))
        weights = jnp.exp(scores - maxima)
        totals = lax.optimization_barrier(jnp.sum(weights, -1))
        rounded = lax.optimization_barrier(weights.astype(jnp.bfloat16)).astype(jnp.float32)
        summed = jnp.einsum('hgqk,khd->qhgd', rounded, value_head_rows)
        return summed / jnp.transpose(totals, (2, 0, 1))[..., None]
    attended = lax.map(attend, query_block_list).reshape(sequence_length, QUERY_HEADS * HEAD_SIZE).astype(jnp.bfloat16)
    mixed_sum = sum_partials(attended, out_weight)
    normed = layer_norm(ALPHA * residual.astype(jnp.float32) + mixed_sum, ln1_gain, ln1_bias).astype(jnp.bfloat16)
    up_acts = jnp.dot(normed, up_weight, preferred_element_type=jnp.float32)
    hidden = jnp.square(jnp.maximum(up_acts, 0.0)).astype(jnp.bfloat16)
    ffn_out = sum_partials(hidden, down_weight)
    return layer_norm(ALPHA * normed.astype(jnp.float32) + ffn_out, ln2_gain, ln2_bias).astype(jnp.bfloat16)
```

```python
import functools
import math

import jax
import jax.numpy as jnp
from jax import lax
from jax.experimental import pallas as pl
from jax.experimental.pallas import tpu as pltpu
from jax.sharding import Mesh, PartitionSpec as P

D = 2048
HEAD_SIZE = 64
GRID_W = 64


ALPHA = 8.0**0.25
ROTARY_BASE = 10000.0
RMS_EPSILON = 1e-06
NORM_EPSILON = 1e-05


def rotate_grid(heads_in, grid_places):
    half_dim = heads_in.shape[-1] // 2
    quarter = half_dim // 2
    inverse = ROTARY_BASE ** (-jnp.arange(quarter, dtype=jnp.float32) / quarter)

    def spin(segment, coords):
        angles = coords.astype(jnp.float32)[:, None] * inverse[None, :]
        cos_val = jnp.cos(angles)[:, None, :]
        sin_val = jnp.sin(angles)[:, None, :]
        lead_half = segment[..., :quarter]
        tail_half = segment[..., quarter:]
        return jnp.concatenate(
            [lead_half * cos_val - tail_half * sin_val, tail_half * cos_val + lead_half * sin_val],
            -1,
        )

    return jnp.concatenate(
        [
            spin(heads_in[..., :half_dim], grid_places // GRID_W),
            spin(heads_in[..., half_dim:], grid_places % GRID_W),
        ],
        -1,
    )


def prepare_inputs(heads_in, gain_vec, grid_places, factor):
    values32 = heads_in.astype(jnp.float32)
    normed = (
        values32
        * lax.rsqrt(jnp.mean(values32 * values32, -1, keepdims=True) + RMS_EPSILON)
        * gain_vec
    )
    return (rotate_grid(normed, grid_places) * factor).astype(jnp.bfloat16)


def layer_norm(pre_norm, gain_vec, bias_vec):
    row_mean = jnp.mean(pre_norm, -1, keepdims=True)
    centred = pre_norm - row_mean
    spread = jnp.mean(centred * centred, -1, keepdims=True)
    return centred * lax.rsqrt(spread + NORM_EPSILON) * gain_vec + bias_vec


def attend_kernel(chunk, q_ref, kv_ref, out_ref, vals_ref):
    width = 2 * HEAD_SIZE
    key_count = kv_ref.shape[0]
    rows = q_ref.shape[0]

    @pl.when(pl.program_id(1) == 0)
    def _():
        lane_kv = lax.broadcasted_iota(jnp.int32, (chunk, width), 1)

        @pl.loop(0, key_count // chunk)
        def _(c):
            at = pl.ds(pl.multiple_of(c * chunk, chunk), chunk)
            vals_ref[at, :] = jnp.where(
                lane_kv < HEAD_SIZE, 1.0, kv_ref[at, :].astype(jnp.float32)
            ).astype(jnp.bfloat16)

    lane = lax.broadcasted_iota(jnp.int32, (rows, width), 1)
    both = q_ref[...].astype(jnp.float32)
    results = []
    for head in range(2):
        own = both if head == 0 else pltpu.roll(both, HEAD_SIZE, 1)
        q = jnp.where(lane < HEAD_SIZE, own, 0.0).astype(jnp.bfloat16)
        top = None
        for c in range(key_count // chunk):
            at = pl.ds(c * chunk, chunk)
            scores = lax.dot_general(
                q, kv_ref[at, :], (((1,), (1,)), ((), ())), preferred_element_type=jnp.float32
            )
            peak = jnp.max(scores, -1, keepdims=True)
            new_top = peak if top is None else jnp.maximum(top, peak)
            weights = jnp.exp(scores - new_top).astype(jnp.bfloat16)
            part = jnp.dot(weights, vals_ref[at, :], preferred_element_type=jnp.float32)
            total = part if top is None else total * jnp.exp(top - new_top) + part
            top = new_top
        results.append(total)
    first, second = (t / pltpu.roll(t, HEAD_SIZE, 1) for t in results)
    out_ref[...] = jnp.where(
        lane < HEAD_SIZE, pltpu.roll(first, HEAD_SIZE, 1), second
    ).astype(jnp.bfloat16)


def attend(q, kv, block=256, chunk=2048):
    heads, rows, width = q.shape
    key_count = kv.shape[1]
    block, chunk = math.gcd(rows, block), math.gcd(key_count, chunk)
    return pl.pallas_call(
        functools.partial(attend_kernel, chunk),
        grid=(heads, rows // block),
        in_specs=[
            pl.BlockSpec((None, block, width), lambda h, i: (h, i, 0)),
            pl.BlockSpec((None, key_count, width), lambda h, i: (h, 0, 0)),
        ],
        out_specs=pl.BlockSpec((None, block, width), lambda h, i: (h, i, 0)),
        out_shape=jax.ShapeDtypeStruct(q.shape, jnp.bfloat16),
        scratch_shapes=[pltpu.VMEM((key_count, width), jnp.bfloat16)],
        compiler_params=pltpu.CompilerParams(dimension_semantics=("arbitrary", "arbitrary")),
        cost_estimate=pl.CostEstimate(
            flops=heads * rows * key_count * 16 * HEAD_SIZE,
            bytes_accessed=2 * (2 * q.size + kv.size),
            transcendentals=heads * rows * key_count * 2,
        ),
    )(q, kv)


def local(
    queries,
    keys,
    values,
    q_gain,
    key_norm_gain,
    out_weight,
    residual,
    ln1_gain,
    ln1_bias,
    up_weight,
    down_weight,
    ln2_gain,
    ln2_bias,
):
    tok_rows = queries.shape[0]
    n_a, n_tp = lax.axis_size("a"), lax.axis_size("tp")
    grid_places = lax.axis_index(("w", "a")) * tok_rows + jnp.arange(tok_rows, dtype=jnp.int32)
    kv_heads = keys.shape[1] // HEAD_SIZE
    q_count = queries.shape[1] // HEAD_SIZE
    own_heads = kv_heads // n_a
    query_rows = prepare_inputs(
        queries.reshape(tok_rows, q_count, HEAD_SIZE), q_gain, grid_places, HEAD_SIZE ** (-0.5)
    ).reshape(tok_rows, kv_heads, 2 * HEAD_SIZE)
    key_rows = prepare_inputs(
        keys.reshape(tok_rows, kv_heads, HEAD_SIZE), key_norm_gain, grid_places, 1.0
    )
    value_rows = values.reshape(tok_rows, kv_heads, HEAD_SIZE)
    packed = jnp.concatenate([query_rows, key_rows, value_rows], -1)
    packed = jnp.transpose(packed, (1, 0, 2)).reshape(n_a, own_heads, tok_rows, 4 * HEAD_SIZE)
    packed = lax.all_to_all(packed, "a", 0, 0, tiled=True)
    packed = jnp.transpose(packed, (1, 0, 2, 3)).reshape(
        own_heads, n_a * tok_rows, 4 * HEAD_SIZE
    )
    q = packed[..., : 2 * HEAD_SIZE]
    kv = lax.all_gather(packed[..., 2 * HEAD_SIZE :], "w", axis=1, tiled=True)

    out_full = lax.all_gather(out_weight, "tp", axis=0, tiled=True)
    up_own = lax.all_to_all(up_weight, "a", 1, 0, tiled=True)
    up_full = lax.all_gather(up_own, "w", axis=0, tiled=True)
    down_own = lax.all_to_all(down_weight, "a", 0, 1, tiled=True)
    down_full = lax.all_gather(down_own, "w", axis=0)

    attended = attend(q, kv)
    rows = tok_rows // n_tp
    sent = attended.reshape(own_heads, n_a * n_tp, rows, 2 * HEAD_SIZE)
    sent = jnp.transpose(sent, (1, 0, 2, 3))
    got = lax.all_to_all(sent, ("a", "tp"), 0, 0, tiled=True)
    got = got.reshape(n_a, n_tp, own_heads, rows, 2 * HEAD_SIZE)
    group_cols = jnp.transpose(got, (1, 3, 0, 2, 4)).reshape(n_tp, rows, -1)
    out_groups = out_full.reshape(2, -1, D)
    both = jnp.transpose(group_cols, (1, 0, 2)).reshape(rows, 2, -1)
    mixed = sum(
        jnp.dot(both[:, g], out_groups[g], preferred_element_type=jnp.float32)
        .astype(jnp.bfloat16)
        .astype(jnp.float32)
        for g in range(2)
    )
    own_residual = lax.dynamic_slice_in_dim(residual, lax.axis_index("tp") * rows, rows, 0)
    normed = layer_norm(
        ALPHA * own_residual.astype(jnp.float32) + mixed, ln1_gain, ln1_bias
    ).astype(jnp.bfloat16)
    full_rows = lax.all_gather(normed, ("a", "tp"), axis=0, tiled=True)
    up_acts = jnp.dot(full_rows, up_full, preferred_element_type=jnp.float32)
    hidden = jnp.square(jnp.maximum(up_acts, 0.0)).astype(jnp.bfloat16)
    partial_ffn = jnp.concatenate(
        [
            jnp.dot(hidden, down_full[i], preferred_element_type=jnp.float32).astype(jnp.bfloat16)
            for i in range(down_full.shape[0])
        ],
        -1,
    )
    ffn_out = lax.psum_scatter(
        partial_ffn, ("a", "tp"), scatter_dimension=0, tiled=True
    ).astype(jnp.float32)
    encoded = layer_norm(
        ALPHA * normed.astype(jnp.float32) + ffn_out, ln2_gain, ln2_bias
    ).astype(jnp.bfloat16)
    return lax.all_to_all(encoded, "tp", 1, 0, tiled=True)


def solution(mesh):
    n_sp, n_tp = mesh.shape["sp"], mesh.shape["tp"]

    def layer(queries, keys, *others):
        n_a = math.gcd(n_sp, keys.shape[1] // (HEAD_SIZE * n_tp))
        groups = Mesh(mesh.devices.reshape(n_sp // n_a, n_a, n_tp), ("w", "a", "tp"))
        sp = ("w", "a")
        cut = P(sp, "tp")
        return jax.shard_map(
            local,
            mesh=groups,
            in_specs=(cut, cut, cut, P(), P(), P("tp", None), P(sp, None), P(), P())
            + (cut, P("tp", sp), P(), P()),
            out_specs=cut,
            check_vma=False,
        )(queries, keys, *others)

    return layer
```

```python
import functools
import math

import jax
import jax.numpy as jnp
from jax import lax
from jax.experimental import pallas as pl
from jax.experimental.pallas import tpu as pltpu
from jax.sharding import Mesh, PartitionSpec as P

D = 2048
HEAD_SIZE = 64
GRID_W = 64


ALPHA = 8.0**0.25
ROTARY_BASE = 10000.0
RMS_EPSILON = 1e-06
NORM_EPSILON = 1e-05


def rotate_grid(heads_in, grid_places):
    half_dim = heads_in.shape[-1] // 2
    quarter = half_dim // 2
    inverse = ROTARY_BASE ** (-jnp.arange(quarter, dtype=jnp.float32) / quarter)

    def spin(segment, coords):
        angles = coords.astype(jnp.float32)[:, None] * inverse[None, :]
        cos_val = jnp.cos(angles)[:, None, :]
        sin_val = jnp.sin(angles)[:, None, :]
        lead_half = segment[..., :quarter]
        tail_half = segment[..., quarter:]
        return jnp.concatenate(
            [lead_half * cos_val - tail_half * sin_val, tail_half * cos_val + lead_half * sin_val],
            -1,
        )

    return jnp.concatenate(
        [
            spin(heads_in[..., :half_dim], grid_places // GRID_W),
            spin(heads_in[..., half_dim:], grid_places % GRID_W),
        ],
        -1,
    )


def prepare_inputs(heads_in, gain_vec, grid_places, factor):
    values32 = heads_in.astype(jnp.float32)
    normed = (
        values32
        * lax.rsqrt(jnp.mean(values32 * values32, -1, keepdims=True) + RMS_EPSILON)
        * gain_vec
    )
    return (rotate_grid(normed, grid_places) * factor).astype(jnp.bfloat16)


def layer_norm(pre_norm, gain_vec, bias_vec):
    row_mean = jnp.mean(pre_norm, -1, keepdims=True)
    centred = pre_norm - row_mean
    spread = jnp.mean(centred * centred, -1, keepdims=True)
    return centred * lax.rsqrt(spread + NORM_EPSILON) * gain_vec + bias_vec


def attend_kernel(chunk, q_ref, kv_ref, out_ref, vals_ref):
    width = 2 * HEAD_SIZE
    key_count = kv_ref.shape[0]
    rows = q_ref.shape[0]

    @pl.when(pl.program_id(1) == 0)
    def _():
        lane_kv = lax.broadcasted_iota(jnp.int32, (chunk, width), 1)

        @pl.loop(0, key_count // chunk)
        def _(c):
            at = pl.ds(pl.multiple_of(c * chunk, chunk), chunk)
            vals_ref[at, :] = jnp.where(
                lane_kv < HEAD_SIZE, 1.0, kv_ref[at, :].astype(jnp.float32)
            ).astype(jnp.bfloat16)

    lane = lax.broadcasted_iota(jnp.int32, (rows, width), 1)
    both = q_ref[...].astype(jnp.float32)
    results = []
    for head in range(2):
        own = both if head == 0 else pltpu.roll(both, HEAD_SIZE, 1)
        q = jnp.where(lane < HEAD_SIZE, own, 0.0).astype(jnp.bfloat16)
        top = None
        for c in range(key_count // chunk):
            at = pl.ds(c * chunk, chunk)
            scores = lax.dot_general(
                q, kv_ref[at, :], (((1,), (1,)), ((), ())), preferred_element_type=jnp.float32
            )
            peak = jnp.max(scores, -1, keepdims=True)
            new_top = peak if top is None else jnp.maximum(top, peak)
            weights = jnp.exp(scores - new_top).astype(jnp.bfloat16)
            part = jnp.dot(weights, vals_ref[at, :], preferred_element_type=jnp.float32)
            total = part if top is None else total * jnp.exp(top - new_top) + part
            top = new_top
        results.append(total)
    first, second = (t / pltpu.roll(t, HEAD_SIZE, 1) for t in results)
    out_ref[...] = jnp.where(
        lane < HEAD_SIZE, pltpu.roll(first, HEAD_SIZE, 1), second
    ).astype(jnp.bfloat16)


def attend(q, kv, block=256, chunk=2048):
    heads, rows, width = q.shape
    key_count = kv.shape[1]
    block, chunk = math.gcd(rows, block), math.gcd(key_count, chunk)
    return pl.pallas_call(
        functools.partial(attend_kernel, chunk),
        grid=(heads, rows // block),
        in_specs=[
            pl.BlockSpec((None, block, width), lambda h, i: (h, i, 0)),
            pl.BlockSpec((None, key_count, width), lambda h, i: (h, 0, 0)),
        ],
        out_specs=pl.BlockSpec((None, block, width), lambda h, i: (h, i, 0)),
        out_shape=jax.ShapeDtypeStruct(q.shape, jnp.bfloat16),
        scratch_shapes=[pltpu.VMEM((key_count, width), jnp.bfloat16)],
        compiler_params=pltpu.CompilerParams(dimension_semantics=("arbitrary", "arbitrary")),
        cost_estimate=pl.CostEstimate(
            flops=heads * rows * key_count * 16 * HEAD_SIZE,
            bytes_accessed=2 * (2 * q.size + kv.size),
            transcendentals=heads * rows * key_count * 2,
        ),
    )(q, kv)


def local(
    queries,
    keys,
    values,
    q_gain,
    key_norm_gain,
    out_weight,
    residual,
    ln1_gain,
    ln1_bias,
    up_weight,
    down_weight,
    ln2_gain,
    ln2_bias,
):
    tok_rows = queries.shape[0]
    n_a, n_tp = lax.axis_size("a"), lax.axis_size("tp")
    grid_places = lax.axis_index(("a", "w")) * tok_rows + jnp.arange(tok_rows, dtype=jnp.int32)
    kv_heads = keys.shape[1] // HEAD_SIZE
    q_count = queries.shape[1] // HEAD_SIZE
    own_heads = kv_heads // n_a
    query_rows = prepare_inputs(
        queries.reshape(tok_rows, q_count, HEAD_SIZE), q_gain, grid_places, HEAD_SIZE ** (-0.5)
    ).reshape(tok_rows, kv_heads, 2 * HEAD_SIZE)
    key_rows = prepare_inputs(
        keys.reshape(tok_rows, kv_heads, HEAD_SIZE), key_norm_gain, grid_places, 1.0
    )
    value_rows = values.reshape(tok_rows, kv_heads, HEAD_SIZE)
    packed = jnp.concatenate([query_rows, key_rows, value_rows], -1)
    packed = jnp.transpose(packed, (1, 0, 2)).reshape(n_a, own_heads, tok_rows, 4 * HEAD_SIZE)
    packed = lax.all_to_all(packed, "a", 0, 0, tiled=True)
    packed = jnp.transpose(packed, (1, 0, 2, 3)).reshape(
        own_heads, n_a * tok_rows, 4 * HEAD_SIZE
    )
    q = packed[..., : 2 * HEAD_SIZE]
    kv = lax.all_gather(packed[..., 2 * HEAD_SIZE :], "w", axis=1, tiled=True)

    out_full = lax.all_gather(out_weight, "tp", axis=0, tiled=True)
    up_own = lax.all_to_all(up_weight, "a", 1, 0, tiled=True)
    up_full = lax.all_gather(up_own, "w", axis=0, tiled=True)
    down_own = lax.all_to_all(down_weight, "a", 0, 1, tiled=True)
    down_full = lax.all_gather(down_own, "w", axis=0)

    attended = attend(q, kv)
    rows = tok_rows // n_tp
    sent = attended.reshape(own_heads, n_a * n_tp, rows, 2 * HEAD_SIZE)
    sent = jnp.transpose(sent, (1, 0, 2, 3))
    got = lax.all_to_all(sent, ("a", "tp"), 0, 0, tiled=True)
    got = got.reshape(n_a, n_tp, own_heads, rows, 2 * HEAD_SIZE)
    group_cols = jnp.transpose(got, (1, 3, 0, 2, 4)).reshape(n_tp, rows, -1)
    out_groups = out_full.reshape(2, -1, D)
    both = jnp.transpose(group_cols, (1, 0, 2)).reshape(rows, 2, -1)
    mixed = sum(
        jnp.dot(both[:, g], out_groups[g], preferred_element_type=jnp.float32)
        .astype(jnp.bfloat16)
        .astype(jnp.float32)
        for g in range(2)
    )
    own_residual = lax.dynamic_slice_in_dim(residual, lax.axis_index("tp") * rows, rows, 0)
    normed = layer_norm(
        ALPHA * own_residual.astype(jnp.float32) + mixed, ln1_gain, ln1_bias
    ).astype(jnp.bfloat16)
    n_w = lax.axis_size("w")
    turned = normed.reshape(rows, n_a, n_w, -1).swapaxes(1, 2).reshape(rows, D)
    full_rows = lax.all_gather(turned, ("a", "tp"), axis=0, tiled=True)
    up_acts = jnp.dot(full_rows, up_full, preferred_element_type=jnp.float32)
    hidden = jnp.square(jnp.maximum(up_acts, 0.0)).astype(jnp.bfloat16)
    partial_ffn = jnp.concatenate(
        [
            jnp.dot(hidden, down_full[i], preferred_element_type=jnp.float32).astype(jnp.bfloat16)
            for i in range(down_full.shape[0])
        ],
        -1,
    )
    ffn_out = lax.psum_scatter(
        partial_ffn, ("a", "tp"), scatter_dimension=0, tiled=True
    )
    ffn_out = (
        ffn_out.reshape(rows, n_w, n_a, -1).swapaxes(1, 2).reshape(rows, D).astype(jnp.float32)
    )
    encoded = layer_norm(
        ALPHA * normed.astype(jnp.float32) + ffn_out, ln2_gain, ln2_bias
    ).astype(jnp.bfloat16)
    return lax.all_to_all(encoded, "tp", 1, 0, tiled=True)


def solution(mesh):
    n_sp, n_tp = mesh.shape["sp"], mesh.shape["tp"]

    def layer(queries, keys, *others):
        n_a = math.gcd(n_sp, keys.shape[1] // (HEAD_SIZE * n_tp))
        groups = Mesh(mesh.devices.reshape(n_a, n_sp // n_a, n_tp), ("a", "w", "tp"))
        sp = ("a", "w")
        cut = P(sp, "tp")
        return jax.shard_map(
            local,
            mesh=groups,
            in_specs=(cut, cut, cut, P(), P(), P("tp", None), P(sp, None), P(), P())
            + (cut, P("tp", sp), P(), P()),
            out_specs=cut,
            check_vma=False,
        )(queries, keys, *others)

    return layer
```

```python
import functools
import math

import jax
import jax.numpy as jnp
from jax import lax
from jax.experimental import pallas as pl
from jax.experimental.pallas import tpu as pltpu
from jax.sharding import Mesh, PartitionSpec as P

D = 2048
HEAD_SIZE = 64
GRID_W = 64


ALPHA = 8.0**0.25
ROTARY_BASE = 10000.0
RMS_EPSILON = 1e-06
NORM_EPSILON = 1e-05


def rotate_grid(heads_in, grid_places):
    half_dim = heads_in.shape[-1] // 2
    quarter = half_dim // 2
    inverse = ROTARY_BASE ** (-jnp.arange(quarter, dtype=jnp.float32) / quarter)

    def spin(segment, coords):
        angles = coords.astype(jnp.float32)[:, None] * inverse[None, :]
        cos_val = jnp.cos(angles)[:, None, :]
        sin_val = jnp.sin(angles)[:, None, :]
        lead_half = segment[..., :quarter]
        tail_half = segment[..., quarter:]
        return jnp.concatenate(
            [lead_half * cos_val - tail_half * sin_val, tail_half * cos_val + lead_half * sin_val],
            -1,
        )

    return jnp.concatenate(
        [
            spin(heads_in[..., :half_dim], grid_places // GRID_W),
            spin(heads_in[..., half_dim:], grid_places % GRID_W),
        ],
        -1,
    )


def prepare_inputs(heads_in, gain_vec, grid_places, factor):
    values32 = heads_in.astype(jnp.float32)
    normed = (
        values32
        * lax.rsqrt(jnp.mean(values32 * values32, -1, keepdims=True) + RMS_EPSILON)
        * gain_vec
    )
    return (rotate_grid(normed, grid_places) * factor).astype(jnp.bfloat16)


def layer_norm(pre_norm, gain_vec, bias_vec):
    row_mean = jnp.mean(pre_norm, -1, keepdims=True)
    centred = pre_norm - row_mean
    spread = jnp.mean(centred * centred, -1, keepdims=True)
    return centred * lax.rsqrt(spread + NORM_EPSILON) * gain_vec + bias_vec


def line_gather(block, axis):
    n, me = lax.axis_size(axis), lax.axis_index(axis)
    up = [(i, i + 1) for i in range(n - 1)]
    down = [(i + 1, i) for i in range(n - 1)]
    from_left, from_right = [block], [block]
    for _ in range(n - 1):
        from_left.append(lax.ppermute(from_left[-1], axis, up))
        from_right.append(lax.ppermute(from_right[-1], axis, down))
    stacked = jnp.zeros((n, *block.shape), block.dtype)
    for k in range(n):
        piece = block if k == 0 else jnp.where(me >= k, from_left[k], from_right[n - k])
        stacked = lax.dynamic_update_index_in_dim(stacked, piece, (me - k + n) % n, 0)
    return stacked


def swap_blocks(blocks, axis):
    n, me = lax.axis_size(axis), lax.axis_index(axis)
    stacked = jnp.zeros_like(blocks)
    for k in range(n):
        piece = lax.dynamic_index_in_dim(blocks, (me + k) % n, 0, keepdims=False)
        if k:
            piece = lax.ppermute(piece, axis, [(i, (i + k) % n) for i in range(n)])
        stacked = lax.dynamic_update_index_in_dim(stacked, piece, (me - k + n) % n, 0)
    return stacked


def attend_kernel(chunk, q_ref, kv_ref, out_ref, vals_ref):
    width = 2 * HEAD_SIZE
    key_count = kv_ref.shape[0]
    rows = q_ref.shape[0]

    @pl.when(pl.program_id(1) == 0)
    def _():
        lane_kv = lax.broadcasted_iota(jnp.int32, (chunk, width), 1)

        @pl.loop(0, key_count // chunk)
        def _(c):
            at = pl.ds(pl.multiple_of(c * chunk, chunk), chunk)
            vals_ref[at, :] = jnp.where(
                lane_kv < HEAD_SIZE, 1.0, kv_ref[at, :].astype(jnp.float32)
            ).astype(jnp.bfloat16)

    lane = lax.broadcasted_iota(jnp.int32, (rows, width), 1)
    both = q_ref[...].astype(jnp.float32)
    results = []
    for head in range(2):
        own = both if head == 0 else pltpu.roll(both, HEAD_SIZE, 1)
        q = jnp.where(lane < HEAD_SIZE, own, 0.0).astype(jnp.bfloat16)
        top = None
        for c in range(key_count // chunk):
            at = pl.ds(c * chunk, chunk)
            scores = lax.dot_general(
                q, kv_ref[at, :], (((1,), (1,)), ((), ())), preferred_element_type=jnp.float32
            )
            peak = jnp.max(scores, -1, keepdims=True)
            new_top = peak if top is None else jnp.maximum(top, peak)
            weights = jnp.exp(scores - new_top).astype(jnp.bfloat16)
            part = jnp.dot(weights, vals_ref[at, :], preferred_element_type=jnp.float32)
            total = part if top is None else total * jnp.exp(top - new_top) + part
            top = new_top
        results.append(total)
    first, second = (t / pltpu.roll(t, HEAD_SIZE, 1) for t in results)
    out_ref[...] = jnp.where(
        lane < HEAD_SIZE, pltpu.roll(first, HEAD_SIZE, 1), second
    ).astype(jnp.bfloat16)


def attend(q, kv, block=256, chunk=2048):
    heads, rows, width = q.shape
    key_count = kv.shape[1]
    block, chunk = math.gcd(rows, block), math.gcd(key_count, chunk)
    return pl.pallas_call(
        functools.partial(attend_kernel, chunk),
        grid=(heads, rows // block),
        in_specs=[
            pl.BlockSpec((None, block, width), lambda h, i: (h, i, 0)),
            pl.BlockSpec((None, key_count, width), lambda h, i: (h, 0, 0)),
        ],
        out_specs=pl.BlockSpec((None, block, width), lambda h, i: (h, i, 0)),
        out_shape=jax.ShapeDtypeStruct(q.shape, jnp.bfloat16),
        scratch_shapes=[pltpu.VMEM((key_count, width), jnp.bfloat16)],
        compiler_params=pltpu.CompilerParams(dimension_semantics=("arbitrary", "arbitrary")),
        cost_estimate=pl.CostEstimate(
            flops=heads * rows * key_count * 16 * HEAD_SIZE,
            bytes_accessed=2 * (2 * q.size + kv.size),
            transcendentals=heads * rows * key_count * 2,
        ),
    )(q, kv)


def local(
    queries,
    keys,
    values,
    q_gain,
    key_norm_gain,
    out_weight,
    residual,
    ln1_gain,
    ln1_bias,
    up_weight,
    down_weight,
    ln2_gain,
    ln2_bias,
):
    tok_rows = queries.shape[0]
    n_a, n_tp = lax.axis_size("a"), lax.axis_size("tp")
    grid_places = lax.axis_index(("a", "w")) * tok_rows + jnp.arange(tok_rows, dtype=jnp.int32)
    kv_heads = keys.shape[1] // HEAD_SIZE
    q_count = queries.shape[1] // HEAD_SIZE
    own_heads = kv_heads // n_a
    query_rows = prepare_inputs(
        queries.reshape(tok_rows, q_count, HEAD_SIZE), q_gain, grid_places, HEAD_SIZE ** (-0.5)
    ).reshape(tok_rows, kv_heads, 2 * HEAD_SIZE)
    key_rows = prepare_inputs(
        keys.reshape(tok_rows, kv_heads, HEAD_SIZE), key_norm_gain, grid_places, 1.0
    )
    value_rows = values.reshape(tok_rows, kv_heads, HEAD_SIZE)
    packed = jnp.concatenate([query_rows, key_rows, value_rows], -1)
    packed = jnp.transpose(packed, (1, 0, 2)).reshape(n_a, own_heads, tok_rows, 4 * HEAD_SIZE)
    packed = lax.all_to_all(packed, "a", 0, 0, tiled=True)
    packed = jnp.transpose(packed, (1, 0, 2, 3)).reshape(
        own_heads, n_a * tok_rows, 4 * HEAD_SIZE
    )
    packed, down_weight = lax.optimization_barrier((packed, down_weight))
    q = packed[..., : 2 * HEAD_SIZE]
    kv = lax.all_gather(packed[..., 2 * HEAD_SIZE :], "w", axis=1, tiled=True)

    out_full = line_gather(out_weight, "tp").reshape(-1, D)
    up_own = lax.all_to_all(up_weight, "a", 1, 0, tiled=True)
    up_full = lax.all_gather(up_own, "w", axis=0, tiled=True)
    down_own = swap_blocks(down_weight.reshape(n_a, -1, down_weight.shape[1]), "a")
    down_own = down_own.swapaxes(0, 1).reshape(down_weight.shape[0] // n_a, -1)

    attended = attend(q, kv)
    rows = tok_rows // n_tp
    sent = attended.reshape(own_heads, n_a * n_tp, rows, 2 * HEAD_SIZE)
    sent = jnp.transpose(sent, (1, 0, 2, 3))
    got = lax.all_to_all(sent, ("a", "tp"), 0, 0, tiled=True)
    got, down_own = lax.optimization_barrier((got, down_own))
    down_full = lax.all_gather(down_own, "w", axis=0)
    got = got.reshape(n_a, n_tp, own_heads, rows, 2 * HEAD_SIZE)
    group_cols = jnp.transpose(got, (1, 3, 0, 2, 4)).reshape(n_tp, rows, -1)
    out_groups = out_full.reshape(2, -1, D)
    both = jnp.transpose(group_cols, (1, 0, 2)).reshape(rows, 2, -1)
    mixed = sum(
        jnp.dot(both[:, g], out_groups[g], preferred_element_type=jnp.float32)
        .astype(jnp.bfloat16)
        .astype(jnp.float32)
        for g in range(2)
    )
    own_residual = lax.dynamic_slice_in_dim(residual, lax.axis_index("tp") * rows, rows, 0)
    normed = layer_norm(
        ALPHA * own_residual.astype(jnp.float32) + mixed, ln1_gain, ln1_bias
    ).astype(jnp.bfloat16)
    n_w = lax.axis_size("w")
    turned = normed.reshape(rows, n_a, n_w, -1).swapaxes(1, 2).reshape(rows, D)
    full_rows = line_gather(line_gather(turned, "a"), "tp").reshape(-1, D)
    up_acts = jnp.dot(full_rows, up_full, preferred_element_type=jnp.float32)
    hidden = jnp.square(jnp.maximum(up_acts, 0.0)).astype(jnp.bfloat16)
    partial_ffn = jnp.concatenate(
        [
            jnp.dot(hidden, down_full[i], preferred_element_type=jnp.float32).astype(jnp.bfloat16)
            for i in range(down_full.shape[0])
        ],
        -1,
    )
    ffn_out = lax.psum_scatter(partial_ffn, "tp", scatter_dimension=0, tiled=True)
    ffn_out = lax.psum_scatter(ffn_out, "a", scatter_dimension=0, tiled=True)
    ffn_out = (
        ffn_out.reshape(rows, n_w, n_a, -1).swapaxes(1, 2).reshape(rows, D).astype(jnp.float32)
    )
    encoded = layer_norm(
        ALPHA * normed.astype(jnp.float32) + ffn_out, ln2_gain, ln2_bias
    ).astype(jnp.bfloat16)
    return lax.all_to_all(encoded, "tp", 1, 0, tiled=True)


def solution(mesh):
    n_sp, n_tp = mesh.shape["sp"], mesh.shape["tp"]

    def layer(queries, keys, *others):
        n_a = math.gcd(n_sp, keys.shape[1] // (HEAD_SIZE * n_tp))
        groups = Mesh(mesh.devices.reshape(n_a, n_sp // n_a, n_tp), ("a", "w", "tp"))
        sp = ("a", "w")
        cut = P(sp, "tp")
        return jax.shard_map(
            local,
            mesh=groups,
            in_specs=(cut, cut, cut, P(), P(), P("tp", None), P(sp, None), P(), P())
            + (cut, P("tp", sp), P(), P()),
            out_specs=cut,
            check_vma=False,
        )(queries, keys, *others)

    return layer
```

```python
import functools
import math

import jax
import jax.numpy as jnp
from jax import lax
from jax.experimental import pallas as pl
from jax.experimental.pallas import tpu as pltpu
from jax.sharding import Mesh, PartitionSpec as P

D = 2048
HEAD_SIZE = 64
GRID_W = 64


ALPHA = 8.0**0.25
ROTARY_BASE = 10000.0
RMS_EPSILON = 1e-06
NORM_EPSILON = 1e-05


def rotate_grid(heads_in, grid_places):
    half_dim = heads_in.shape[-1] // 2
    quarter = half_dim // 2
    inverse = ROTARY_BASE ** (-jnp.arange(quarter, dtype=jnp.float32) / quarter)

    def spin(segment, coords):
        angles = coords.astype(jnp.float32)[:, None] * inverse[None, :]
        cos_val = jnp.cos(angles)[:, None, :]
        sin_val = jnp.sin(angles)[:, None, :]
        lead_half = segment[..., :quarter]
        tail_half = segment[..., quarter:]
        return jnp.concatenate(
            [lead_half * cos_val - tail_half * sin_val, tail_half * cos_val + lead_half * sin_val],
            -1,
        )

    return jnp.concatenate(
        [
            spin(heads_in[..., :half_dim], grid_places // GRID_W),
            spin(heads_in[..., half_dim:], grid_places % GRID_W),
        ],
        -1,
    )


def prepare_inputs(heads_in, gain_vec, grid_places, factor):
    values32 = heads_in.astype(jnp.float32)
    normed = (
        values32
        * lax.rsqrt(jnp.mean(values32 * values32, -1, keepdims=True) + RMS_EPSILON)
        * gain_vec
    )
    return (rotate_grid(normed, grid_places) * factor).astype(jnp.bfloat16)


def layer_norm(pre_norm, gain_vec, bias_vec):
    row_mean = jnp.mean(pre_norm, -1, keepdims=True)
    centred = pre_norm - row_mean
    spread = jnp.mean(centred * centred, -1, keepdims=True)
    return centred * lax.rsqrt(spread + NORM_EPSILON) * gain_vec + bias_vec


def line_gather(block, axis):
    n, me = lax.axis_size(axis), lax.axis_index(axis)
    up = [(i, i + 1) for i in range(n - 1)]
    down = [(i + 1, i) for i in range(n - 1)]
    from_left, from_right = [block], [block]
    for _ in range(n - 1):
        from_left.append(lax.ppermute(from_left[-1], axis, up))
        from_right.append(lax.ppermute(from_right[-1], axis, down))
    stacked = jnp.zeros((n, *block.shape), block.dtype)
    for k in range(n):
        piece = block if k == 0 else jnp.where(me >= k, from_left[k], from_right[n - k])
        stacked = lax.dynamic_update_index_in_dim(stacked, piece, (me - k + n) % n, 0)
    return stacked


def swap_blocks(blocks, axis):
    n, me = lax.axis_size(axis), lax.axis_index(axis)
    stacked = jnp.zeros_like(blocks)
    for k in range(n):
        piece = lax.dynamic_index_in_dim(blocks, (me + k) % n, 0, keepdims=False)
        if k:
            piece = lax.ppermute(piece, axis, [(i, (i + k) % n) for i in range(n)])
        stacked = lax.dynamic_update_index_in_dim(stacked, piece, (me - k + n) % n, 0)
    return stacked


def turn_cols(block, outer, inner):
    width = block.shape[1] // (outer * inner)
    starts = [(o * inner + i) * width for i in range(inner) for o in range(outer)]
    return jnp.concatenate([block[:, c : c + width] for c in starts], -1)


def attend_kernel(chunk, q_ref, kv_ref, out_ref, vals_ref):
    width = 2 * HEAD_SIZE
    key_count = kv_ref.shape[0]
    rows = q_ref.shape[0]

    @pl.when(pl.program_id(1) == 0)
    def _():
        lane_kv = lax.broadcasted_iota(jnp.int32, (chunk, width), 1)

        @pl.loop(0, key_count // chunk)
        def _(c):
            at = pl.ds(pl.multiple_of(c * chunk, chunk), chunk)
            vals_ref[at, :] = jnp.where(
                lane_kv < HEAD_SIZE, 1.0, kv_ref[at, :].astype(jnp.float32)
            ).astype(jnp.bfloat16)

    lane = lax.broadcasted_iota(jnp.int32, (rows, width), 1)
    both = q_ref[...].astype(jnp.float32)
    results = []
    for head in range(2):
        own = both if head == 0 else pltpu.roll(both, HEAD_SIZE, 1)
        q = jnp.where(lane < HEAD_SIZE, own, 0.0).astype(jnp.bfloat16)
        top = None
        for c in range(key_count // chunk):
            at = pl.ds(c * chunk, chunk)
            scores = lax.dot_general(
                q, kv_ref[at, :], (((1,), (1,)), ((), ())), preferred_element_type=jnp.float32
            )
            peak = jnp.max(scores, -1, keepdims=True)
            new_top = peak if top is None else jnp.maximum(top, peak)
            weights = jnp.exp(scores - new_top).astype(jnp.bfloat16)
            part = jnp.dot(weights, vals_ref[at, :], preferred_element_type=jnp.float32)
            total = part if top is None else total * jnp.exp(top - new_top) + part
            top = new_top
        results.append(total)
    first, second = (t / pltpu.roll(t, HEAD_SIZE, 1) for t in results)
    out_ref[...] = jnp.where(
        lane < HEAD_SIZE, pltpu.roll(first, HEAD_SIZE, 1), second
    ).astype(jnp.bfloat16)


def attend(q, kv, block=256, chunk=2048):
    heads, rows, width = q.shape
    key_count = kv.shape[1]
    block, chunk = math.gcd(rows, block), math.gcd(key_count, chunk)
    return pl.pallas_call(
        functools.partial(attend_kernel, chunk),
        grid=(heads, rows // block),
        in_specs=[
            pl.BlockSpec((None, block, width), lambda h, i: (h, i, 0)),
            pl.BlockSpec((None, key_count, width), lambda h, i: (h, 0, 0)),
        ],
        out_specs=pl.BlockSpec((None, block, width), lambda h, i: (h, i, 0)),
        out_shape=jax.ShapeDtypeStruct(q.shape, jnp.bfloat16),
        scratch_shapes=[pltpu.VMEM((key_count, width), jnp.bfloat16)],
        compiler_params=pltpu.CompilerParams(dimension_semantics=("arbitrary", "arbitrary")),
        cost_estimate=pl.CostEstimate(
            flops=heads * rows * key_count * 16 * HEAD_SIZE,
            bytes_accessed=2 * (2 * q.size + kv.size),
            transcendentals=heads * rows * key_count * 2,
        ),
    )(q, kv)


def local(
    queries,
    keys,
    values,
    q_gain,
    key_norm_gain,
    out_weight,
    residual,
    ln1_gain,
    ln1_bias,
    up_weight,
    down_weight,
    ln2_gain,
    ln2_bias,
):
    tok_rows = queries.shape[0]
    n_a, n_tp = lax.axis_size("a"), lax.axis_size("tp")
    grid_places = lax.axis_index(("a", "w")) * tok_rows + jnp.arange(tok_rows, dtype=jnp.int32)
    kv_heads = keys.shape[1] // HEAD_SIZE
    q_count = queries.shape[1] // HEAD_SIZE
    own_heads = kv_heads // n_a
    query_rows = prepare_inputs(
        queries.reshape(tok_rows, q_count, HEAD_SIZE), q_gain, grid_places, HEAD_SIZE ** (-0.5)
    ).reshape(tok_rows, kv_heads, 2 * HEAD_SIZE)
    key_rows = prepare_inputs(
        keys.reshape(tok_rows, kv_heads, HEAD_SIZE), key_norm_gain, grid_places, 1.0
    )
    value_rows = values.reshape(tok_rows, kv_heads, HEAD_SIZE)
    packed = jnp.concatenate([query_rows, key_rows, value_rows], -1)
    packed = jnp.transpose(packed, (1, 0, 2)).reshape(n_a, own_heads, tok_rows, 4 * HEAD_SIZE)
    packed = lax.all_to_all(packed, "a", 0, 0, tiled=True)
    packed = jnp.transpose(packed, (1, 0, 2, 3)).reshape(
        own_heads, n_a * tok_rows, 4 * HEAD_SIZE
    )
    q = packed[..., : 2 * HEAD_SIZE]
    kv = lax.all_gather(packed[..., 2 * HEAD_SIZE :], "w", axis=1, tiled=True)
    kv, down_weight = lax.optimization_barrier((kv, down_weight))

    out_full = line_gather(out_weight, "tp").reshape(-1, D)
    up_own = lax.all_to_all(up_weight, "a", 1, 0, tiled=True)
    up_full = lax.all_gather(up_own, "w", axis=0, tiled=True)
    down_own = swap_blocks(down_weight.reshape(n_a, -1, down_weight.shape[1]), "a")
    down_own = down_own.swapaxes(0, 1).reshape(down_weight.shape[0] // n_a, -1)

    attended = attend(q, kv)
    rows = tok_rows // n_tp
    sent = attended.reshape(own_heads, n_a * n_tp, rows, 2 * HEAD_SIZE)
    sent = jnp.transpose(sent, (1, 0, 2, 3))
    got = lax.all_to_all(sent, ("a", "tp"), 0, 0, tiled=True)
    got, down_own = lax.optimization_barrier((got, down_own))
    down_full = lax.all_gather(down_own, "w", axis=0)
    got = got.reshape(n_a, n_tp, own_heads, rows, 2 * HEAD_SIZE)
    group_cols = jnp.transpose(got, (1, 3, 0, 2, 4)).reshape(n_tp, rows, -1)
    out_groups = out_full.reshape(2, -1, D)
    both = jnp.transpose(group_cols, (1, 0, 2)).reshape(rows, 2, -1)
    mixed = sum(
        jnp.dot(both[:, g], out_groups[g], preferred_element_type=jnp.float32)
        .astype(jnp.bfloat16)
        .astype(jnp.float32)
        for g in range(2)
    )
    own_residual = lax.dynamic_slice_in_dim(residual, lax.axis_index("tp") * rows, rows, 0)
    normed = layer_norm(
        ALPHA * own_residual.astype(jnp.float32) + mixed, ln1_gain, ln1_bias
    ).astype(jnp.bfloat16)
    n_w = lax.axis_size("w")
    turned = turn_cols(normed, n_a, n_w)
    full_rows = line_gather(line_gather(turned, "a"), "tp").reshape(-1, D)
    up_acts = jnp.dot(full_rows, up_full, preferred_element_type=jnp.float32)
    hidden = jnp.square(jnp.maximum(up_acts, 0.0)).astype(jnp.bfloat16)
    partial_ffn = jnp.concatenate(
        [
            jnp.dot(hidden, down_full[i], preferred_element_type=jnp.float32).astype(jnp.bfloat16)
            for i in range(down_full.shape[0])
        ],
        -1,
    )
    ffn_out = lax.psum_scatter(partial_ffn, "tp", scatter_dimension=0, tiled=True)
    ffn_out = lax.psum_scatter(ffn_out, "a", scatter_dimension=0, tiled=True)
    ffn_out = turn_cols(ffn_out, n_w, n_a).astype(jnp.float32)
    encoded = layer_norm(
        ALPHA * normed.astype(jnp.float32) + ffn_out, ln2_gain, ln2_bias
    ).astype(jnp.bfloat16)
    return lax.all_to_all(encoded, "tp", 1, 0, tiled=True)


def solution(mesh):
    n_sp, n_tp = mesh.shape["sp"], mesh.shape["tp"]

    def layer(queries, keys, *others):
        n_a = math.gcd(n_sp, keys.shape[1] // (HEAD_SIZE * n_tp))
        groups = Mesh(mesh.devices.reshape(n_a, n_sp // n_a, n_tp), ("a", "w", "tp"))
        sp = ("a", "w")
        cut = P(sp, "tp")
        return jax.shard_map(
            local,
            mesh=groups,
            in_specs=(cut, cut, cut, P(), P(), P("tp", None), P(sp, None), P(), P())
            + (cut, P("tp", sp), P(), P()),
            out_specs=cut,
            check_vma=False,
        )(queries, keys, *others)

    return layer
```

```python
import functools
import math

import jax
import jax.numpy as jnp
from jax import lax
from jax.experimental import pallas as pl
from jax.experimental.pallas import tpu as pltpu
from jax.sharding import Mesh, PartitionSpec as P

D = 2048
HEAD_SIZE = 64
GRID_W = 64


ALPHA = 8.0**0.25
ROTARY_BASE = 10000.0
RMS_EPSILON = 1e-06
NORM_EPSILON = 1e-05


def rotate_grid(heads_in, grid_places):
    half_dim = heads_in.shape[-1] // 2
    quarter = half_dim // 2
    inverse = ROTARY_BASE ** (-jnp.arange(quarter, dtype=jnp.float32) / quarter)

    def spin(segment, coords):
        angles = coords.astype(jnp.float32)[:, None] * inverse[None, :]
        cos_val = jnp.cos(angles)[:, None, :]
        sin_val = jnp.sin(angles)[:, None, :]
        lead_half = segment[..., :quarter]
        tail_half = segment[..., quarter:]
        return jnp.concatenate(
            [lead_half * cos_val - tail_half * sin_val, tail_half * cos_val + lead_half * sin_val],
            -1,
        )

    return jnp.concatenate(
        [
            spin(heads_in[..., :half_dim], grid_places // GRID_W),
            spin(heads_in[..., half_dim:], grid_places % GRID_W),
        ],
        -1,
    )


def prepare_inputs(heads_in, gain_vec, grid_places, factor):
    values32 = heads_in.astype(jnp.float32)
    normed = (
        values32
        * lax.rsqrt(jnp.mean(values32 * values32, -1, keepdims=True) + RMS_EPSILON)
        * gain_vec
    )
    return (rotate_grid(normed, grid_places) * factor).astype(jnp.bfloat16)


def layer_norm(pre_norm, gain_vec, bias_vec):
    row_mean = jnp.mean(pre_norm, -1, keepdims=True)
    centred = pre_norm - row_mean
    spread = jnp.mean(centred * centred, -1, keepdims=True)
    return centred * lax.rsqrt(spread + NORM_EPSILON) * gain_vec + bias_vec


def line_gather(block, axis):
    n, me = lax.axis_size(axis), lax.axis_index(axis)
    up = [(i, i + 1) for i in range(n - 1)]
    down = [(i + 1, i) for i in range(n - 1)]
    from_left, from_right = [block], [block]
    for _ in range(n - 1):
        from_left.append(lax.ppermute(from_left[-1], axis, up))
        from_right.append(lax.ppermute(from_right[-1], axis, down))
    stacked = jnp.zeros((n, *block.shape), block.dtype)
    for k in range(n):
        piece = block if k == 0 else jnp.where(me >= k, from_left[k], from_right[n - k])
        stacked = lax.dynamic_update_index_in_dim(stacked, piece, (me - k + n) % n, 0)
    return stacked


def swap_blocks(blocks, axis):
    n, me = lax.axis_size(axis), lax.axis_index(axis)
    stacked = jnp.zeros_like(blocks)
    for k in range(n):
        piece = lax.dynamic_index_in_dim(blocks, (me + k) % n, 0, keepdims=False)
        if k:
            piece = lax.ppermute(piece, axis, [(i, (i + k) % n) for i in range(n)])
        stacked = lax.dynamic_update_index_in_dim(stacked, piece, (me - k + n) % n, 0)
    return stacked


def turn_cols(block, outer, inner):
    width = block.shape[1] // (outer * inner)
    starts = [(o * inner + i) * width for i in range(inner) for o in range(outer)]
    return jnp.concatenate([block[:, c : c + width] for c in starts], -1)


def attend_kernel(chunk, q_ref, kv_ref, out_ref, vals_ref):
    width = 2 * HEAD_SIZE
    key_count = kv_ref.shape[0]
    rows = q_ref.shape[0]

    @pl.when(pl.program_id(1) == 0)
    def _():
        lane_kv = lax.broadcasted_iota(jnp.int32, (chunk, width), 1)

        @pl.loop(0, key_count // chunk)
        def _(c):
            at = pl.ds(pl.multiple_of(c * chunk, chunk), chunk)
            vals_ref[at, :] = jnp.where(
                lane_kv < HEAD_SIZE, 1.0, kv_ref[at, :].astype(jnp.float32)
            ).astype(jnp.bfloat16)

    lane = lax.broadcasted_iota(jnp.int32, (rows, width), 1)
    both = q_ref[...].astype(jnp.float32)
    results = []
    for head in range(2):
        own = both if head == 0 else pltpu.roll(both, HEAD_SIZE, 1)
        q = jnp.where(lane < HEAD_SIZE, own, 0.0).astype(jnp.bfloat16)
        top = None
        for c in range(key_count // chunk):
            at = pl.ds(c * chunk, chunk)
            scores = lax.dot_general(
                q, kv_ref[at, :], (((1,), (1,)), ((), ())), preferred_element_type=jnp.float32
            )
            peak = jnp.max(scores, -1, keepdims=True)
            new_top = peak if top is None else jnp.maximum(top, peak)
            weights = jnp.exp(scores - new_top).astype(jnp.bfloat16)
            part = jnp.dot(weights, vals_ref[at, :], preferred_element_type=jnp.float32)
            total = part if top is None else total * jnp.exp(top - new_top) + part
            top = new_top
        results.append(total)
    first, second = (t / pltpu.roll(t, HEAD_SIZE, 1) for t in results)
    out_ref[...] = jnp.where(
        lane < HEAD_SIZE, pltpu.roll(first, HEAD_SIZE, 1), second
    ).astype(jnp.bfloat16)


def attend(q, kv, block=256, chunk=2048):
    heads, rows, width = q.shape
    key_count = kv.shape[1]
    block, chunk = math.gcd(rows, block), math.gcd(key_count, chunk)
    return pl.pallas_call(
        functools.partial(attend_kernel, chunk),
        grid=(heads, rows // block),
        in_specs=[
            pl.BlockSpec((None, block, width), lambda h, i: (h, i, 0)),
            pl.BlockSpec((None, key_count, width), lambda h, i: (h, 0, 0)),
        ],
        out_specs=pl.BlockSpec((None, block, width), lambda h, i: (h, i, 0)),
        out_shape=jax.ShapeDtypeStruct(q.shape, jnp.bfloat16),
        scratch_shapes=[pltpu.VMEM((key_count, width), jnp.bfloat16)],
        compiler_params=pltpu.CompilerParams(dimension_semantics=("arbitrary", "arbitrary")),
        cost_estimate=pl.CostEstimate(
            flops=heads * rows * key_count * 16 * HEAD_SIZE,
            bytes_accessed=2 * (2 * q.size + kv.size),
            transcendentals=heads * rows * key_count * 2,
        ),
    )(q, kv)


def local(
    queries,
    keys,
    values,
    q_gain,
    key_norm_gain,
    out_weight,
    residual,
    ln1_gain,
    ln1_bias,
    up_weight,
    down_weight,
    ln2_gain,
    ln2_bias,
):
    tok_rows = queries.shape[0]
    n_a, n_tp = lax.axis_size("a"), lax.axis_size("tp")
    grid_places = lax.axis_index(("a", "w")) * tok_rows + jnp.arange(tok_rows, dtype=jnp.int32)
    kv_heads = keys.shape[1] // HEAD_SIZE
    q_count = queries.shape[1] // HEAD_SIZE
    own_heads = kv_heads // n_a
    query_rows = prepare_inputs(
        queries.reshape(tok_rows, q_count, HEAD_SIZE), q_gain, grid_places, HEAD_SIZE ** (-0.5)
    ).reshape(tok_rows, kv_heads, 2 * HEAD_SIZE)
    key_rows = prepare_inputs(
        keys.reshape(tok_rows, kv_heads, HEAD_SIZE), key_norm_gain, grid_places, 1.0
    )
    value_rows = values.reshape(tok_rows, kv_heads, HEAD_SIZE)
    packed = jnp.concatenate([query_rows, key_rows, value_rows], -1)
    packed = jnp.transpose(packed, (1, 0, 2)).reshape(n_a, own_heads, tok_rows, 4 * HEAD_SIZE)
    packed = lax.all_to_all(packed, "a", 0, 0, tiled=True)
    packed = jnp.transpose(packed, (1, 0, 2, 3)).reshape(
        own_heads, n_a * tok_rows, 4 * HEAD_SIZE
    )
    q = packed[..., : 2 * HEAD_SIZE]
    kv = lax.all_gather(packed[..., 2 * HEAD_SIZE :], "w", axis=1, tiled=True)
    kv, down_weight = lax.optimization_barrier((kv, down_weight))

    out_full = line_gather(out_weight, "tp").reshape(-1, D)
    up_own = lax.all_to_all(up_weight, "a", 1, 0, tiled=True)
    up_full = lax.all_gather(up_own, "w", axis=0, tiled=True)
    down_own = swap_blocks(down_weight.reshape(n_a, -1, down_weight.shape[1]), "a")
    down_own = down_own.swapaxes(0, 1).reshape(down_weight.shape[0] // n_a, -1)

    attended = attend(q, kv)
    rows = tok_rows // n_tp
    sent = attended.reshape(own_heads, n_a * n_tp, rows, 2 * HEAD_SIZE)
    sent = jnp.transpose(sent, (1, 0, 2, 3))
    got = lax.all_to_all(sent, ("a", "tp"), 0, 0, tiled=True)
    got, down_own = lax.optimization_barrier((got, down_own))
    down_full = lax.all_gather(down_own, "w", axis=0)
    got = got.reshape(n_a, n_tp, own_heads, rows, 2 * HEAD_SIZE)
    group_cols = jnp.transpose(got, (1, 3, 0, 2, 4)).reshape(n_tp, rows, -1)
    out_groups = out_full.reshape(2, -1, D)
    both = jnp.transpose(group_cols, (1, 0, 2)).reshape(rows, 2, -1)
    mixed = sum(
        jnp.dot(both[:, g], out_groups[g], preferred_element_type=jnp.float32)
        .astype(jnp.bfloat16)
        .astype(jnp.float32)
        for g in range(2)
    )
    own_residual = lax.dynamic_slice_in_dim(residual, lax.axis_index("tp") * rows, rows, 0)
    normed = layer_norm(
        ALPHA * own_residual.astype(jnp.float32) + mixed, ln1_gain, ln1_bias
    ).astype(jnp.bfloat16)
    n_w = lax.axis_size("w")
    turned = turn_cols(normed, n_a, n_w)
    full_rows = line_gather(line_gather(turned, "a"), "tp").reshape(-1, D)
    up_acts = jnp.dot(full_rows, up_full, preferred_element_type=jnp.float32)
    hidden = jnp.square(jnp.maximum(up_acts, 0.0)).astype(jnp.bfloat16)
    partial_ffn = jnp.concatenate(
        [
            jnp.dot(hidden, down_full[i], preferred_element_type=jnp.float32).astype(jnp.bfloat16)
            for i in range(down_full.shape[0])
        ],
        -1,
    )
    ffn_out = lax.psum_scatter(partial_ffn, "tp", scatter_dimension=0, tiled=True)
    ffn_out = lax.psum_scatter(ffn_out, "a", scatter_dimension=0, tiled=True)
    ffn_out = (
        ffn_out.reshape(rows, n_w, n_a, -1).swapaxes(1, 2).reshape(rows, D).astype(jnp.float32)
    )
    encoded = layer_norm(
        ALPHA * normed.astype(jnp.float32) + ffn_out, ln2_gain, ln2_bias
    ).astype(jnp.bfloat16)
    return lax.all_to_all(encoded, "tp", 1, 0, tiled=True)


def solution(mesh):
    n_sp, n_tp = mesh.shape["sp"], mesh.shape["tp"]

    def layer(queries, keys, *others):
        n_a = math.gcd(n_sp, keys.shape[1] // (HEAD_SIZE * n_tp))
        groups = Mesh(mesh.devices.reshape(n_a, n_sp // n_a, n_tp), ("a", "w", "tp"))
        sp = ("a", "w")
        cut = P(sp, "tp")
        return jax.shard_map(
            local,
            mesh=groups,
            in_specs=(cut, cut, cut, P(), P(), P("tp", None), P(sp, None), P(), P())
            + (cut, P("tp", sp), P(), P()),
            out_specs=cut,
            check_vma=False,
        )(queries, keys, *others)

    return layer
```
